32 devices in a mesh: ep: 8 (over z, x), tp: 4 (over y, core).
Axes of the slice: x: 2, y: 2, z: 4, core: 2. Of those that a mesh axis runs over, the one named last changes fastest.
Arguments:
- out_gate: bfloat16 [8192, 1024], P('ep', 'tp'), may hold values from -6 to 6
- in_gate: bfloat16 [8192, 1024], P('ep', 'tp'), may hold values from -6 to 6
- conv_input: bfloat16 [8192, 1024], P('ep', 'tp'), may hold values from -6 to 6
- conv_taps: float32 [3, 1024], P(None, 'tp'), may hold values from -4 to 4
- group_gain: float32 [1024], P('tp'), may hold values from 0.1 to 1.9
- mix_out_w: bfloat16 [1024, 2048], replicated, may hold values from -0.1875 to 0.1875
- moe_in: bfloat16 [8192, 2048], P(('ep', 'tp')), may hold values from -6 to 6
- moe_gain: float32 [2048], replicated, may hold values from 0.1 to 1.9
- route_ids: int32 [8192, 2], P(('ep', 'tp')), may hold values from 0 to 31, as said below
- route_weight: float32 [8192, 2], P(('ep', 'tp')), may hold values from 0.1 to 1
- gate_w: bfloat16 [32, 2048, 1024], P(('ep', 'tp')), may hold values from -0.125 to 0.125
- up_w: bfloat16 [32, 2048, 1024], P(('ep', 'tp')), may hold values from -0.125 to 0.125
- down_w: bfloat16 [32, 1024, 2048], P(('ep', 'tp')), may hold values from -0.1875 to 0.1875
Outputs:
- mixed: bfloat16 [8192, 2048], P(('ep', 'tp'))
- moe_out: bfloat16 [8192, 2048], P(('ep', 'tp'))
The draws below stay inside these ranges and needn't reach their ends.
Inputs may be any that keep to these rules, and one draw needn't show every extreme that they name: `route_ids`: the two numbers of a row are different experts of one group: group g holds experts g * 4 to g * 4 + 3. The rows of one device (aligned blocks of 256 rows) name each group in exactly 32 rows and each expert in exactly 16 rows.
All inputs are finite; a program needn't handle non-finite values.
Results may differ from the reference program's by a relative error of at most 0.0071.
Values may be sent and summed in bfloat16 or wider, within the bound.
No kernel may reach another device: no remote copies, remote signals or barrier semaphores. Data moves between devices by JAX's collectives and lax.ppermute only.
A program may use at most 128 MiB of HBM per device.

```python
import jax
import jax.numpy as jnp
from jax import lax

D = 2048
CC = 1024
GROUP_CH = 64
TAPS = 3
FE = 1024
TOK_B = 256
GROUPS = 8
EXP_GROUP = 4
EXPERTS = 32
TOKENS_A = 8192
TOKENS_B = 8192


def draw_route_ids(key, part):
    block_count = TOKENS_B // TOK_B
    per_group = TOK_B // GROUPS
    block_keys = jax.random.split(jax.random.fold_in(key, 11), block_count)

    def one_block(block_key):
        order_key, label_key = jax.random.split(block_key)
        slot_of = jax.random.permutation(order_key, TOK_B).astype(jnp.int32)
        group_of = slot_of // per_group
        inner_slot = slot_of % per_group
        first_pick = inner_slot % EXP_GROUP
        shift_by = 1 + inner_slot // EXP_GROUP % (EXP_GROUP - 1)
        second_pick = (first_pick + shift_by) % EXP_GROUP
        label_keys = jax.random.split(label_key, GROUPS)
        labels = jax.vmap(lambda one_key: jax.random.permutation(one_key, EXP_GROUP))(label_keys).astype(jnp.int32)
        first_id = group_of * EXP_GROUP + labels[group_of, first_pick]
        second_id = group_of * EXP_GROUP + labels[group_of, second_pick]
        return jnp.stack([first_id, second_id], axis=1)
    return jax.vmap(one_block)(block_keys).reshape(TOKENS_B, 2).astype(jnp.int32)


def block_scale(own_key, extent, cuts, low, largest):
    loudness, own = 1.0, jax.random.fold_in(own_key, 6)
    for dim, parts in cuts:
        draws = jnp.exp(jax.random.uniform(jax.random.fold_in(own, dim), (parts,), jnp.float32, low / len(cuts), largest / len(cuts)))
        loudness = loudness * jnp.repeat(draws, extent[dim] // parts).reshape([-1 if axis == dim else 1 for axis in range(len(extent))])
    return loudness


def centred(own_key, shape, deviation, bound, pieces=(), dtype=jnp.bfloat16):
    drawn = deviation * jax.random.normal(own_key, shape, jnp.float32)
    if pieces:
        drawn = drawn * block_scale(own_key, shape, pieces, -0.22, 0.18)
    return jnp.clip(drawn, -bound, bound).astype(dtype)


def setup_inputs(seed: int = 0) -> dict:
    keys = jax.random.split(jax.random.key(seed), 14)
    return {
        "out_gate": centred(keys[0], (TOKENS_A, CC), 1.0, 6.0, ((0, 8), (1, 4))),
        "in_gate": centred(keys[1], (TOKENS_A, CC), 1.0, 6.0, ((0, 8), (1, 4))),
        "conv_input": centred(keys[2], (TOKENS_A, CC), 1.0, 6.0, ((0, 8), (1, 4))),
        "conv_taps": centred(keys[3], (TAPS, CC), 0.577, 4.0, ((1, 4),), jnp.float32),
        "group_gain": jnp.clip(1.0 + 0.18 * jax.random.normal(keys[4], (CC,), jnp.float32), 0.1, 1.9),
        "mix_out_w": centred(keys[5], (CC, D), CC ** -0.5, 0.1875),
        "moe_in": centred(keys[6], (TOKENS_B, D), 1.0, 6.0, ((0, 32),)),
        "moe_gain": jnp.clip(1.0 + 0.18 * jax.random.normal(keys[7], (D,), jnp.float32), 0.1, 1.9),
        "route_ids": draw_route_ids(jax.random.fold_in(keys[13], 71), 0),
        "route_weight": jnp.clip(0.1 + 0.9 * jax.random.uniform(keys[9], (TOKENS_B, 2), jnp.float32) ** block_scale(keys[9], (TOKENS_B, 2), ((0, 32),), -0.2, 0.2), 0.1, 1.0),
        "gate_w": centred(keys[10], (EXPERTS, D, FE), D ** -0.5, 0.125, ((0, 32),)),
        "up_w": centred(keys[11], (EXPERTS, D, FE), D ** -0.5, 0.125, ((0, 32),)),
        "down_w": centred(keys[12], (EXPERTS, FE, D), FE ** -0.5, 0.1875, ((0, 32),)),
    }


def conv_mixer(out_gate, in_gate, conv_input, conv_taps, group_gain, mix_out_w):
    product = in_gate.astype(jnp.float32) * conv_input.astype(jnp.float32)
    length = product.shape[0]
    padded = jnp.pad(product, ((TAPS - 1, 0), (0, 0)))
    convolved = jnp.zeros_like(product)
    for tap in range(TAPS):
        convolved = convolved + conv_taps[tap] * padded[tap:tap + length]
    gated = out_gate.astype(jnp.float32) * convolved
    grouped = gated.reshape(length, CC // GROUP_CH, GROUP_CH)
    inv_rms = lax.rsqrt(lax.optimization_barrier(jnp.mean(grouped * grouped, axis=-1, keepdims=True)) + 1e-06)
    normed = ((grouped * inv_rms).reshape(length, CC) * group_gain).astype(jnp.bfloat16)
    return jnp.dot(normed, mix_out_w, preferred_element_type=jnp.float32).astype(jnp.bfloat16)

def expert_rows(inputs, w_gate, w_up, w_down):
    gate_part = jnp.dot(inputs, w_gate, preferred_element_type=jnp.float32)
    up_part = jnp.dot(inputs, w_up, preferred_element_type=jnp.float32)
    hidden = (jax.nn.silu(gate_part) * up_part).astype(jnp.bfloat16)
    return jnp.dot(hidden, w_down, preferred_element_type=jnp.float32).astype(jnp.bfloat16)

def reference(out_gate, in_gate, conv_input, conv_taps, group_gain, mix_out_w, moe_in, moe_gain, route_ids, route_weight, gate_w, up_w, down_w):
    mixed = conv_mixer(out_gate, in_gate, conv_input, conv_taps, group_gain, mix_out_w)
    wide_in = moe_in.astype(jnp.float32)
    inv_rms = lax.rsqrt(lax.optimization_barrier(jnp.mean(wide_in * wide_in, axis=-1, keepdims=True)) + 1e-06)
    expert_in = (wide_in * inv_rms * moe_gain).astype(jnp.bfloat16)
    flat_ids = route_ids.reshape(-1).astype(jnp.int32)
    sort_order = jnp.argsort(flat_ids).astype(jnp.int32)
    per_expert = flat_ids.shape[0] // EXPERTS
    tokens_of = (sort_order // 2).reshape(EXPERTS, per_expert)

    def one_expert(operands):
        token_rows, w_gate, w_up, w_down = operands
        return expert_rows(expert_in[token_rows], w_gate, w_up, w_down)
    outputs = lax.map(one_expert, (tokens_of, gate_w, up_w, down_w))
    per_assign = jnp.zeros((flat_ids.shape[0], D), jnp.bfloat16).at[sort_order].set(outputs.reshape(-1, D))
    per_assign = per_assign.reshape(-1, 2, D)
    first_out = per_assign[:, 0].astype(jnp.float32)
    second = per_assign[:, 1].astype(jnp.float32)
    moe_out = (first_out * route_weight[:, 0:1] + second * route_weight[:, 1:2]).astype(jnp.bfloat16)
    return (mixed, moe_out)
```

```python
import functools

import jax
import jax.numpy as jnp
from jax import lax
from jax.experimental import pallas as pl
from jax.experimental.pallas import tpu as pltpu
from jax.sharding import PartitionSpec as P

GROUP_CH = 64
LANES = 128
META = 16
EPS = 1e-06
F32 = jnp.float32
BF16 = jnp.bfloat16


VMEM = pl.BlockSpec(memory_space=pltpu.VMEM)
SMEM = pl.BlockSpec(memory_space=pltpu.SMEM)


def dot(a, b):
    return jnp.dot(a, b, preferred_element_type=F32)


def dot_nt(a, b):
    return lax.dot_general(a, b, (((1,), (1,)), ((), ())), preferred_element_type=F32)


def iota(shape, dim):
    return lax.broadcasted_iota(jnp.int32, shape, dim)


def call(body, outs, specs, args, scratch, flops, name, vmem):
    return pl.pallas_call(
        body,
        out_shape=outs,
        in_specs=specs,
        out_specs=jax.tree.map(lambda _: VMEM, outs),
        scratch_shapes=scratch,
        cost_estimate=pl.CostEstimate(flops=flops, bytes_accessed=1 << 20, transcendentals=0),
        compiler_params=pltpu.CompilerParams(vmem_limit_bytes=vmem << 20),
        name=name,
    )(*args)


def swap(value, axis, mask):
    count = lax.axis_size(axis)
    return lax.ppermute(value, axis, [(i, i ^ mask) for i in range(count)])


def prep_body(sizes, where, x_own, x_mate, route_own, route_mate, gain, *refs):
    groups, members, per_group, width = sizes
    chunks, pos_out, normed = refs[:-2], refs[-2], refs[-1]
    me, core = where[0], where[2]
    tokens = x_own.shape[0]
    step = min(64, tokens)
    for side, x_ref in enumerate((x_own, x_mate)):

        def rows(r, carry, x_ref=x_ref, side=side):
            start = pl.multiple_of(r * step, step)
            wide = x_ref[pl.ds(start, step), :].astype(F32)
            scale = lax.rsqrt(jnp.mean(wide * wide, axis=-1, keepdims=True) + EPS)
            normed[pl.ds(pl.multiple_of(side * tokens + start, step), step), :width] = (
                wide * scale * gain[...]
            ).astype(BF16)
            return carry

        lax.fori_loop(0, tokens // step, rows, 0)
    experts = -(-groups * members // 16) * 16
    before = (iota((tokens, tokens), 0) < iota((tokens, tokens), 1)).astype(BF16)
    ident = (iota((tokens, tokens), 0) == iota((tokens, tokens), 1)).astype(BF16)
    places = []
    for side, route in enumerate((route_own, route_mate)):
        first = route[0:1, :].astype(jnp.int32)
        second = route[1:2, :].astype(jnp.int32)
        lane = iota((experts, tokens), 0)
        one, two = lane == first, lane == second
        seen = dot((one | two).astype(BF16), before)
        rank_one = jnp.sum(jnp.where(one, seen, 0.0), axis=0, keepdims=True)
        rank_two = jnp.sum(jnp.where(two, seen, 0.0), axis=0, keepdims=True)
        group = first // members
        rank = (jnp.sum(jnp.where(lane // members == group, seen, 0.0), axis=0, keepdims=True) * 0.5).astype(jnp.int32)
        mask = jnp.bitwise_xor(group, me)
        mine = jnp.bitwise_and(mask, 1) == core
        base = (mask // 2) * (2 * per_group) + rank
        places.append(jnp.where(mine, base + side * per_group, -1))
        if side == 0:
            half = groups * per_group
            back = jnp.where(mine, base, half + base + per_group).astype(F32)
            pos_out[...] = jnp.broadcast_to(back, (LANES, tokens)).T
        parts = []
        for k in range(2):
            left = route[2 + k : 3 + k, :]
            for _ in range(3):
                part = left.astype(BF16).astype(F32)
                parts.append(part)
                left = left - part
        row = iota((META, tokens), 0)
        meta = jnp.zeros((META, tokens), F32)
        fields = [(first % members).astype(F32), rank_one, (second % members).astype(F32), rank_two, *parts]
        for at, field in enumerate(fields):
            meta = jnp.where(row == at, field, meta)
        spread = (iota((LANES, META), 0) == iota((LANES, META), 1)).astype(BF16)
        flat = dot(spread, meta.astype(BF16)).astype(BF16)
        normed[pl.ds(side * tokens, tokens), width:] = dot_nt(ident, flat).astype(BF16)
    place = jnp.concatenate(places, axis=1)
    total = groups * per_group
    pick = (iota((total, 2 * tokens), 0) == place).astype(BF16)
    block = width // 4
    size = 2 * per_group

    def columns(n, carry):
        cols = pl.ds(pl.multiple_of(n * block, LANES), block)
        out = dot(pick, normed[:, cols]).astype(BF16)
        for k, ref in enumerate(chunks):
            ref[:, cols] = out[k * size : (k + 1) * size]
        return carry

    lax.fori_loop(0, 4, columns, 0)
    out = dot(pick, normed[:, width:]).astype(BF16)
    for k, ref in enumerate(chunks):
        ref[:, width:] = out[k * size : (k + 1) * size]


def expert_body(sizes, where, *refs):
    members, per_group, per_expert, width, count = sizes
    landed = [refs[m * count : (m + 1) * count] for m in range(members)]
    gate, up, down = refs[members * count : members * count + 3]
    outs, rows_x, hidden = refs[members * count + 3 : -2], refs[-2], refs[-1]
    me = where[1]
    size = 2 * per_group
    span = count * 2 * per_expert
    block = 512
    pick_row = (iota((META, LANES), 0) == iota((META, LANES), 1)).astype(BF16)
    for m in range(members):
        lanes = jnp.concatenate([r[:, width:] for r in landed[m]], axis=0)
        meta = dot_nt(pick_row, lanes).astype(jnp.int32)
        n = iota((1, count * size), 1)
        base = (n // size) * (2 * per_expert) + ((n % size) // per_group) * per_expert
        at = jnp.where(meta[0:1] == me, base + meta[1:2], jnp.where(meta[2:3] == me, base + meta[3:4], -1))
        pick = (iota((span, count * size), 0) == at).astype(BF16)
        for n in range(width // block):
            cols = slice(n * block, (n + 1) * block)
            value = jnp.concatenate([r[:, cols] for r in landed[m]], axis=0)
            rows_x[m * span : (m + 1) * span, cols] = dot(pick, value).astype(BF16)
    inner = hidden.shape[1]
    wide = 256

    def first(n, carry):
        cols = pl.ds(pl.multiple_of(n * wide, wide), wide)
        gated = dot(rows_x[...], gate[0, :, cols])
        upper = dot(rows_x[...], up[0, :, cols])
        hidden[:, cols] = (gated / (1.0 + jnp.exp(-gated)) * upper).astype(BF16)
        return carry

    lax.fori_loop(0, inner // wide, first, 0)

    def second(n, carry):
        cols = pl.ds(pl.multiple_of(n * wide, wide), wide)
        out = dot(hidden[...], down[0, :, cols]).astype(BF16)
        outs[0][:, cols] = out[:span]
        outs[1][:, cols] = out[span : 2 * span]
        for m in range(2, members, 2):
            outs[1 + m // 2][:, cols] = out[m * span : (m + 2) * span]
        return carry

    lax.fori_loop(0, width // wide, second, 0)


def combine_body(sizes, where, *refs):
    members, per_group, per_expert, width, count = sizes
    metas, sources, outs = refs[:count], refs[count:-count], refs[-count:]
    me = where[1]
    size = 2 * per_group
    span = count * 2 * per_expert
    rows = count * size
    lanes = jnp.concatenate([r[:, width:] for r in metas], axis=0).astype(F32)
    n = iota((rows, 1), 0)
    base = (n // size) * (2 * per_expert) + ((n % size) // per_group) * per_expert
    depth = sum(r.shape[0] for r in sources)
    column = iota((rows, depth), 1)
    picks, weights = [], []
    for k in range(2):
        mask = jnp.bitwise_xor(lanes[:, 2 * k : 2 * k + 1].astype(jnp.int32), me)
        rank = lanes[:, 2 * k + 1 : 2 * k + 2].astype(jnp.int32)
        even = mask - jnp.bitwise_and(mask, 1)
        odd = jnp.bitwise_and(mask, 1)
        at = jnp.where(even == 0, odd * span, (2 * even - 2 + 3 * odd) * span)
        picks.append((column == at + base + rank).astype(BF16))
        w = 4 + 3 * k
        weights.append(lanes[:, w : w + 1] + lanes[:, w + 1 : w + 2] + lanes[:, w + 2 : w + 3])
    block = 512
    for c in range(width // block):
        cols = slice(c * block, (c + 1) * block)
        value = jnp.concatenate([r[:, cols] for r in sources], axis=0)
        out = (dot(picks[0], value) * weights[0] + dot(picks[1], value) * weights[1]).astype(BF16)
        for k, ref in enumerate(outs):
            ref[:, cols] = out[k * size : (k + 1) * size]


def final_body(pos, *refs):
    sources, out = refs[:-1], refs[-1]
    depth = sum(r.shape[0] for r in sources)
    tokens, width = out.shape
    pick = (iota((tokens, depth), 1) == pos[:, 0:1].astype(jnp.int32)).astype(BF16)
    block = 512
    for c in range(width // block):
        cols = slice(c * block, (c + 1) * block)
        value = jnp.concatenate([r[:, cols] for r in sources], axis=0)
        out[:, cols] = dot(pick, value).astype(BF16)


def conv_body(reach, where, out_gate, in_gate, conv_input, edge, taps, gain, *refs):
    outs, product, normed = refs[:-2], refs[-2], refs[-1]
    me = where[1]
    rows, channels = in_gate.shape
    lead = edge.shape[0] // 2
    product[:lead] = edge[:lead].astype(F32) * edge[lead:].astype(F32)
    step = min(128, rows)
    share = (iota((channels, channels), 0) // GROUP_CH == iota((channels, channels), 1) // GROUP_CH).astype(F32) / GROUP_CH
    for r in range(rows // step):
        at = slice(r * step, (r + 1) * step)
        product[lead + r * step : lead + (r + 1) * step] = in_gate[at].astype(F32) * conv_input[at].astype(F32)
    for r in range(rows // step):
        at = slice(r * step, (r + 1) * step)
        total = None
        for tap in range(reach + 1):
            low = lead - reach + tap + r * step
            term = taps[tap : tap + 1, :] * product[low : low + step]
            total = term if total is None else total + term
        gated = out_gate[at].astype(F32) * total
        mean = jnp.dot(gated * gated, share, preferred_element_type=F32, precision=lax.Precision.HIGHEST)
        normed[at] = (gated * lax.rsqrt(mean + EPS) * gain[...]).astype(BF16)
    part = rows // len(outs)
    for m, ref in enumerate(outs):
        ref[...] = normed[pl.ds(pl.multiple_of(jnp.bitwise_xor(me, m) * part, part), part), :]


def mix_body(where, weight, *refs):
    blocks, out = refs[:-1], refs[-1]
    me = where[1]
    channels = blocks[0].shape[1]
    width = out.shape[1]
    block = 512

    def columns(n, carry):
        cols = pl.ds(pl.multiple_of(n * block, block), block)
        total = None
        for m, ref in enumerate(blocks):
            low = pl.multiple_of(jnp.bitwise_xor(me, m) * channels, channels)
            term = dot(ref[...], weight[pl.ds(low, channels), cols])
            total = term if total is None else total + term
        out[:, cols] = total.astype(BF16)
        return carry

    lax.fori_loop(0, width // block, columns, 0)


def shards(
    out_gate,
    in_gate,
    conv_input,
    conv_taps,
    group_gain,
    mix_out_w,
    moe_in,
    moe_gain,
    route_ids,
    route_weight,
    gate_w,
    up_w,
    down_w,
):
    members, groups = lax.axis_size("tp"), lax.axis_size("ep")
    me_ep, me_tp = lax.axis_index("ep"), lax.axis_index("tp")
    where = jnp.stack([me_ep, me_tp, me_tp % 2]).astype(jnp.int32)
    tokens, width = moe_in.shape
    inner = gate_w.shape[2]
    per_group = tokens // groups
    per_expert = 2 * per_group // members
    full = width + LANES
    size = 2 * per_group
    n_chunks = groups // 2

    rows, channels = in_gate.shape
    reach = conv_taps.shape[0] - 1
    edge = jnp.concatenate([in_gate[rows - 8 :], conv_input[rows - 8 :]], axis=0)
    edge = lax.ppermute(edge, "ep", [(i, i + 1) for i in range(groups - 1)])

    route = jnp.concatenate([route_ids.T.astype(F32), route_weight.T], axis=0)
    route_mate = swap(route, "tp", 1)
    x_mate = swap(moe_in, "tp", 1)
    *leaving, back_pos = call(
        functools.partial(prep_body, (groups, members, per_group, width)),
        [jax.ShapeDtypeStruct((size, full), BF16)] * n_chunks + [jax.ShapeDtypeStruct((tokens, LANES), F32)],
        [SMEM] + [VMEM] * 5,
        (where, moe_in, x_mate, route, route_mate, moe_gain.reshape(1, width)),
        [pltpu.VMEM((2 * tokens, full), BF16)],
        4 * tokens * tokens * width,
        "prep",
        16,
    )

    def across(value, k):
        pairs = []
        for i in range(groups):
            for j in range(members):
                mask = 2 * k + j % 2
                if mask:
                    pairs.append((i * members + j, (i ^ mask) * members + j))
        got = lax.ppermute(value, ("ep", "tp"), pairs)
        return jnp.where(me_tp % 2 == 0, value, got) if k == 0 else got

    halves = [list(range(0, n_chunks, 2)), list(range(1, n_chunks, 2))]
    order = [k for half in halves for k in half]
    landed = {}
    for k in order:
        landed[k, 0] = across(leaving[k], k)
    for k in order:
        landed[k, 1] = swap(landed[k, 0], "tp", 1)
        for m in range(2, members, 2):
            landed[k, m] = swap(landed[k, 0], "tp", m)
            landed[k, m + 1] = swap(landed[k, m], "tp", 1)

    normed = call(
        functools.partial(conv_body, reach),
        [jax.ShapeDtypeStruct((rows // members, channels), BF16)] * members,
        [SMEM] + [VMEM] * 6,
        (where, out_gate, in_gate, conv_input, edge, conv_taps, group_gain.reshape(1, channels)),
        [pltpu.VMEM((rows + 8, channels), F32), pltpu.VMEM((rows, channels), BF16)],
        2 * rows * channels * channels * 8,
        "conv",
        8,
    )
    blocks = [normed[0]] + [swap(normed[m], "tp", m) for m in range(1, members)]
    mixed = call(
        mix_body,
        jax.ShapeDtypeStruct((rows // members, width), BF16),
        [SMEM] + [VMEM] * (1 + members),
        (where, mix_out_w, *blocks),
        [],
        2 * (rows // members) * channels * members * width,
        "mix",
        8,
    )

    returned = {}
    for half in halves:
        count = len(half)
        span = count * 2 * per_expert
        sizes = (members, per_group, per_expert, width, count)
        outs = call(
            functools.partial(expert_body, sizes),
            [jax.ShapeDtypeStruct((span, width), BF16)] * 2
            + [jax.ShapeDtypeStruct((2 * span, width), BF16)] * (members // 2 - 1),
            [SMEM] + [VMEM] * (members * count + 3),
            (where, *[landed[k, m] for m in range(members) for k in half], gate_w, up_w, down_w),
            [pltpu.VMEM((members * span, width), BF16), pltpu.VMEM((members * span, inner), BF16)],
            6 * members * span * width * inner,
            "expert",
            16,
        )
        sources = [outs[0], swap(outs[1], "tp", 1)]
        for m in range(2, members, 2):
            there = swap(outs[1 + m // 2], "tp", m)
            sources += [there, swap(there, "tp", 1)]
        merged = call(
            functools.partial(combine_body, sizes),
            [jax.ShapeDtypeStruct((size, width), BF16)] * count,
            [SMEM] + [VMEM] * (count + len(sources)),
            (where, *[landed[k, 0] for k in half], *sources),
            [],
            4 * count * size * 6 * span * width,
            "combine",
            8,
        )
        for k, value in zip(half, merged):
            returned[k] = across(value, k)
    ordered = [returned[k] for k in range(n_chunks)]
    moe_out = call(
        final_body,
        jax.ShapeDtypeStruct((tokens, width), BF16),
        [VMEM] * (1 + 2 * n_chunks),
        (back_pos, *ordered, *[swap(value, "tp", 1) for value in ordered]),
        [],
        4 * tokens * tokens * width,
        "final",
        8,
    )
    return (mixed, moe_out)


def solution(mesh):
    in_specs = (
        P("ep", "tp"),
        P("ep", "tp"),
        P("ep", "tp"),
        P(None, "tp"),
        P("tp"),
        P(),
        P(("ep", "tp"), None),
        P(),
        P(("ep", "tp"), None),
        P(("ep", "tp"), None),
        P(("ep", "tp"), None, None),
        P(("ep", "tp"), None, None),
        P(("ep", "tp"), None, None),
    )
    out_specs = (P(("ep", "tp"), None), P(("ep", "tp"), None))
    return jax.shard_map(shards, mesh=mesh, in_specs=in_specs, out_specs=out_specs, check_vma=False)
```

```python
import functools

import jax
import jax.numpy as jnp
from jax import lax
from jax.experimental import pallas as pl
from jax.experimental.pallas import tpu as pltpu
from jax.sharding import PartitionSpec as P


GROUP_CH = 64
LANES = 128
META = 16
EPS = 1e-06
F32 = jnp.float32
BF16 = jnp.bfloat16


VMEM = pl.BlockSpec(memory_space=pltpu.VMEM)
SMEM = pl.BlockSpec(memory_space=pltpu.SMEM)
HBM = pl.BlockSpec(memory_space=pltpu.HBM)


def dot(a, b):
    return jnp.dot(a, b, preferred_element_type=F32)


def dot_nt(a, b):
    return lax.dot_general(a, b, (((1,), (1,)), ((), ())), preferred_element_type=F32)


def iota(shape, dim):
    return lax.broadcasted_iota(jnp.int32, shape, dim)


def call(body, outs, specs, args, scratch, flops, vmem):
    return pl.pallas_call(
        body,
        out_shape=outs,
        in_specs=specs,
        out_specs=jax.tree.map(lambda _: VMEM, outs),
        scratch_shapes=scratch,
        cost_estimate=pl.CostEstimate(flops=flops, bytes_accessed=1 << 20, transcendentals=0),
        compiler_params=pltpu.CompilerParams(vmem_limit_bytes=vmem << 20),
    )(*args)


def swap(value, axis, mask):
    count = lax.axis_size(axis)
    return lax.ppermute(value, axis, [(i, i ^ mask) for i in range(count)])


def supers_of(n_chunks):
    return [part for part in (list(range(0, n_chunks, 2)), list(range(1, n_chunks, 2))) if part]


def fetch(pairs, sems):
    copies = [pltpu.make_async_copy(a, b, sems.at[n]) for n, (a, b) in enumerate(pairs)]
    for copy in copies:
        copy.start()
    return copies


def norm_rows(x_ref, gain, normed, width):
    tokens = x_ref.shape[0]
    step = min(64, tokens)

    def rows(r, carry):
        at = pl.ds(pl.multiple_of(r * step, step), step)
        wide = x_ref[at, :].astype(F32)
        scale = lax.rsqrt(jnp.mean(wide * wide, axis=-1, keepdims=True) + EPS)
        normed[at, :width] = (wide * scale * gain[...]).astype(BF16)
        return carry

    lax.fori_loop(0, tokens // step, rows, 0)


def ranks(sizes, ids, me):
    groups, members, per_group, _ = sizes
    tokens = ids.shape[1]
    experts = -(-groups * members // 16) * 16
    first, second = ids[0:1, :], ids[1:2, :]
    before = (iota((tokens, tokens), 0) < iota((tokens, tokens), 1)).astype(BF16)
    lane = iota((experts, tokens), 0)
    one, two = lane == first, lane == second
    seen = dot((one | two).astype(BF16), before)
    rank_one = jnp.sum(jnp.where(one, seen, 0.0), axis=0, keepdims=True)
    rank_two = jnp.sum(jnp.where(two, seen, 0.0), axis=0, keepdims=True)
    group = first // members
    rank = jnp.sum(jnp.where(lane // members == group, seen, 0.0), axis=0, keepdims=True) * 0.5
    mask = jnp.bitwise_xor(group, me)
    return rank_one, rank_two, (mask // 2) * (2 * per_group) + rank.astype(jnp.int32), jnp.bitwise_and(mask, 1)


def route_rows(sizes, ids, weights, normed, me):
    _, members, _, width = sizes
    tokens = normed.shape[0]
    first, second = ids[0:1, :], ids[1:2, :]
    rank_one, rank_two, base, odd = ranks(sizes, ids, me)
    parts = []
    for k in range(2):
        left = weights[k : k + 1, :]
        for _ in range(3):
            part = left.astype(BF16).astype(F32)
            parts.append(part)
            left = left - part
    row = iota((META, tokens), 0)
    meta = jnp.zeros((META, tokens), F32)
    fields = [(first % members).astype(F32), rank_one, (second % members).astype(F32), rank_two, *parts]
    for at, field in enumerate(fields):
        meta = jnp.where(row == at, field, meta)
    spread = (iota((LANES, META), 0) == iota((LANES, META), 1)).astype(BF16)
    flat = dot(spread, meta.astype(BF16)).astype(BF16)
    ident = (iota((tokens, tokens), 0) == iota((tokens, tokens), 1)).astype(BF16)
    normed[:, width:] = dot_nt(ident, flat).astype(BF16)
    return base, odd


def own_body(sizes, where, x, ids, weights, gain, normed, place):
    base, odd = route_rows(sizes, ids, weights, normed, where[0])
    place[...] = jnp.broadcast_to(jnp.where(odd == where[2], base, -1), place.shape)
    norm_rows(x, gain, normed, sizes[3])


def back_body(sizes, where, ids, pos):
    groups, _, per_group, _ = sizes
    _, _, base, odd = ranks(sizes, ids, where[0])
    back = jnp.where(odd == where[2], base, groups * per_group + base + per_group).astype(F32)
    pos[...] = jnp.broadcast_to(back, (pos.shape[1], pos.shape[0])).T


def prep_body(sizes, where, own, place_own, x_mate, ids_mate, weights_mate, gain, *refs):
    groups, _, per_group, width = sizes
    chunks, mate = refs[:-1], refs[-1]
    base, odd = route_rows(sizes, ids_mate, weights_mate, mate, where[0])
    norm_rows(x_mate, gain, mate, width)
    place_mate = jnp.where(odd == where[2], base + per_group, -1)
    total = groups * per_group
    tokens = mate.shape[0]
    picks = [(iota((total, tokens), 0) == place).astype(BF16) for place in (place_own[0:1, :], place_mate)]
    pick = jnp.concatenate(picks, axis=1)
    block = width // 4
    size = 2 * per_group

    def columns(n, carry):
        cols = pl.ds(pl.multiple_of(n * block, LANES), block)
        out = dot(pick, jnp.concatenate([own[:, cols], mate[:, cols]], axis=0)).astype(BF16)
        for k, ref in enumerate(chunks):
            ref[:, cols] = out[k * size : (k + 1) * size]
        return carry

    lax.fori_loop(0, 4, columns, 0)
    out = dot(pick, jnp.concatenate([own[:, width:], mate[:, width:]], axis=0)).astype(BF16)
    for k, ref in enumerate(chunks):
        ref[:, width:] = out[k * size : (k + 1) * size]


def expert_body(sizes, where, *refs):
    members, per_group, per_expert, width, count = sizes
    landed = [refs[m * count : (m + 1) * count] for m in range(members)]
    gate, up, down = refs[members * count : members * count + 3]
    outs, rows_x, hidden = refs[members * count + 3 : -2], refs[-2], refs[-1]
    me = where[1]
    size = 2 * per_group
    span = count * 2 * per_expert
    block = 512
    pick_row = (iota((META, LANES), 0) == iota((META, LANES), 1)).astype(BF16)
    for m in range(members):
        lanes = jnp.concatenate([r[:, width:] for r in landed[m]], axis=0)
        meta = dot_nt(pick_row, lanes).astype(jnp.int32)
        n = iota((1, count * size), 1)
        base = (n // size) * (2 * per_expert) + ((n % size) // per_group) * per_expert
        at = jnp.where(meta[0:1] == me, base + meta[1:2], jnp.where(meta[2:3] == me, base + meta[3:4], -1))
        pick = (iota((span, count * size), 0) == at).astype(BF16)
        for n in range(width // block):
            cols = slice(n * block, (n + 1) * block)
            value = jnp.concatenate([r[:, cols] for r in landed[m]], axis=0)
            rows_x[m * span : (m + 1) * span, cols] = dot(pick, value).astype(BF16)
    gated = dot(rows_x[...], gate[...])
    upper = dot(rows_x[...], up[...])
    hidden[...] = (gated / (1.0 + jnp.exp(-gated)) * upper).astype(BF16)
    out = dot(hidden[...], down[...]).astype(BF16)
    outs[0][...] = out[:span]
    outs[1][...] = out[span : 2 * span]
    for m in range(2, members, 2):
        outs[1 + m // 2][...] = out[m * span : (m + 2) * span]


def fetch_body(*refs):
    count = (len(refs) - 1) // 2
    for copy in fetch(list(zip(refs[:count], refs[count:-1])), refs[-1]):
        copy.wait()


def combine_body(sizes, where, *refs):
    _, per_group, per_expert, width, count = sizes
    metas, sources, outs = refs[:count], refs[count:-count], refs[-count:]
    me = where[1]
    size = 2 * per_group
    span = count * 2 * per_expert
    rows = count * size
    lanes = jnp.concatenate([r[:, width:] for r in metas], axis=0).astype(F32)
    n = iota((rows, 1), 0)
    base = (n // size) * (2 * per_expert) + ((n % size) // per_group) * per_expert
    depth = sum(r.shape[0] for r in sources)
    column = iota((rows, depth), 1)
    picks, weights = [], []
    for k in range(2):
        mask = jnp.bitwise_xor(lanes[:, 2 * k : 2 * k + 1].astype(jnp.int32), me)
        rank = lanes[:, 2 * k + 1 : 2 * k + 2].astype(jnp.int32)
        even = mask - jnp.bitwise_and(mask, 1)
        odd = jnp.bitwise_and(mask, 1)
        at = jnp.where(even == 0, odd * span, (2 * even - 2 + 3 * odd) * span)
        picks.append((column == at + base + rank).astype(BF16))
        w = 4 + 3 * k
        weights.append(lanes[:, w : w + 1] + lanes[:, w + 1 : w + 2] + lanes[:, w + 2 : w + 3])
    block = 512
    for c in range(width // block):
        cols = slice(c * block, (c + 1) * block)
        value = jnp.concatenate([r[:, cols] for r in sources], axis=0)
        out = (dot(picks[0], value) * weights[0] + dot(picks[1], value) * weights[1]).astype(BF16)
        for k, ref in enumerate(outs):
            ref[:, cols] = out[k * size : (k + 1) * size]


def final_body(pos, *refs):
    sources, out = refs[:-1], refs[-1]
    depth = sum(r.shape[0] for r in sources)
    tokens, width = out.shape
    pick = (iota((tokens, depth), 1) == pos[:, 0:1].astype(jnp.int32)).astype(BF16)
    block = 512
    for c in range(width // block):
        cols = slice(c * block, (c + 1) * block)
        value = jnp.concatenate([r[:, cols] for r in sources], axis=0)
        out[:, cols] = dot(pick, value).astype(BF16)


def conv_body(reach, where, edge, *refs):
    given, outs, taken = refs[:5], refs[5:-8], refs[-8:-3]
    product, normed, sems = refs[-3:]
    copies = fetch(list(zip(given, taken)), sems)
    in_gate, conv_input, out_gate, taps, gain = taken
    me = where[1]
    for copy in copies:
        copy.wait()
    rows, channels = in_gate.shape
    lead = edge.shape[0] // 2
    product[:lead] = edge[:lead].astype(F32) * edge[lead:].astype(F32)
    step = min(128, rows)
    share = (iota((channels, channels), 0) // GROUP_CH == iota((channels, channels), 1) // GROUP_CH).astype(F32) / GROUP_CH
    for r in range(rows // step):
        at = slice(r * step, (r + 1) * step)
        product[lead + r * step : lead + (r + 1) * step] = in_gate[at].astype(F32) * conv_input[at].astype(F32)
    for r in range(rows // step):
        at = slice(r * step, (r + 1) * step)
        total = None
        for tap in range(reach + 1):
            low = lead - reach + tap + r * step
            term = taps[tap : tap + 1, :] * product[low : low + step]
            total = term if total is None else total + term
        gated = out_gate[at].astype(F32) * total
        mean = jnp.dot(gated * gated, share, preferred_element_type=F32, precision=lax.Precision.HIGHEST)
        normed[at] = (gated * lax.rsqrt(mean + EPS) * gain[...]).astype(BF16)
    part = rows // len(outs)
    for m, ref in enumerate(outs):
        ref[...] = normed[pl.ds(pl.multiple_of(jnp.bitwise_xor(me, m) * part, part), part), :]


def mix_body(where, weight, *refs):
    blocks, out = refs[:-1], refs[-1]
    me = where[1]
    channels = blocks[0].shape[1]
    width = out.shape[1]
    block = 512

    def columns(n, carry):
        cols = pl.ds(pl.multiple_of(n * block, block), block)
        total = None
        for m, ref in enumerate(blocks):
            low = pl.multiple_of(jnp.bitwise_xor(me, m) * channels, channels)
            term = dot(ref[...], weight[pl.ds(low, channels), cols])
            total = term if total is None else total + term
        out[:, cols] = total.astype(BF16)
        return carry

    lax.fori_loop(0, width // block, columns, 0)


def shards(
    out_gate,
    in_gate,
    conv_input,
    conv_taps,
    group_gain,
    mix_out_w,
    moe_in,
    moe_gain,
    route_ids,
    route_weight,
    gate_w,
    up_w,
    down_w,
):
    members, groups = lax.axis_size("tp"), lax.axis_size("ep")
    me_ep, me_tp = lax.axis_index("ep"), lax.axis_index("tp")
    where = jnp.stack([me_ep, me_tp, me_tp % 2]).astype(jnp.int32)
    tokens, width = moe_in.shape
    inner = gate_w.shape[2]
    per_group = tokens // groups
    per_expert = 2 * per_group // members
    full = width + LANES
    size = 2 * per_group
    n_chunks = groups // 2

    rows, channels = in_gate.shape
    reach = conv_taps.shape[0] - 1

    x_mate = swap(moe_in, "tp", 1)
    ids, ids_mate = route_ids.T, swap(route_ids.T, "tp", 1)
    weights, weights_mate = route_weight.T, swap(route_weight.T, "tp", 1)
    gain = moe_gain.reshape(1, width)
    sizes_all = (groups, members, per_group, width)
    normed, place = call(
        functools.partial(own_body, sizes_all),
        [jax.ShapeDtypeStruct((tokens, full), BF16), jax.ShapeDtypeStruct((8, tokens), jnp.int32)],
        [SMEM] + [VMEM] * 4,
        (where, moe_in, ids, weights, gain),
        [],
        6 << 30,
        16,
    )
    leaving = call(
        functools.partial(prep_body, sizes_all),
        [jax.ShapeDtypeStruct((size, full), BF16)] * n_chunks,
        [SMEM] + [VMEM] * 6,
        (where, normed, place, x_mate, ids_mate, weights_mate, gain),
        [pltpu.VMEM((tokens, full), BF16)],
        20 << 30,
        16,
    )
    edge = jnp.concatenate([in_gate[rows - 8 :], conv_input[rows - 8 :]], axis=0)
    edge = lax.ppermute(edge, "ep", [(i, i + 1) for i in range(groups - 1)])

    def across(value, k):
        pairs = []
        for i in range(groups):
            for j in range(members):
                mask = 2 * k + j % 2
                if mask:
                    pairs.append((i * members + j, (i ^ mask) * members + j))
        got = lax.ppermute(value, ("ep", "tp"), pairs)
        return jnp.where(me_tp % 2 == 0, value, got) if k == 0 else got

    given = (gate_w[0], up_w[0], down_w[0])
    held = call(
        fetch_body,
        [jax.ShapeDtypeStruct(w.shape, BF16) for w in given],
        [HBM] * 3,
        given,
        [pltpu.SemaphoreType.DMA((3,))],
        1 << 30,
        2,
    )
    halves = supers_of(n_chunks)
    order = [k for half in halves for k in half]
    landed = {}
    for k in order:
        landed[k, 0] = across(leaving[k], k)
    for k in order:
        landed[k, 1] = swap(landed[k, 0], "tp", 1)
        for m in range(2, members, 2):
            landed[k, m] = swap(landed[k, 0], "tp", m)
            landed[k, m + 1] = swap(landed[k, m], "tp", 1)

    normed = call(
        functools.partial(conv_body, reach),
        [jax.ShapeDtypeStruct((rows // members, channels), BF16)] * members,
        [SMEM, VMEM] + [HBM] * 5,
        (where, edge, in_gate, conv_input, out_gate, conv_taps, group_gain.reshape(1, channels)),
        [pltpu.VMEM((rows, channels), BF16)] * 3
        + [
            pltpu.VMEM(conv_taps.shape, F32),
            pltpu.VMEM((1, channels), F32),
            pltpu.VMEM((rows + 8, channels), F32),
            pltpu.VMEM((rows, channels), BF16),
            pltpu.SemaphoreType.DMA((5,)),
        ],
        20 << 30,
        8,
    )
    blocks = [normed[0]] + [swap(normed[m], "tp", m) for m in range(1, members)]
    mixed = call(
        mix_body,
        jax.ShapeDtypeStruct((rows // members, width), BF16),
        [SMEM] + [VMEM] * (1 + members),
        (where, mix_out_w, *blocks),
        [],
        2 * (rows // members) * channels * members * width,
        8,
    )

    returned = {}
    for half in halves:
        count = len(half)
        span = count * 2 * per_expert
        sizes = (members, per_group, per_expert, width, count)
        outs = call(
            functools.partial(expert_body, sizes),
            [jax.ShapeDtypeStruct((span, width), BF16)] * 2
            + [jax.ShapeDtypeStruct((2 * span, width), BF16)] * (members // 2 - 1),
            [SMEM] + [VMEM] * (members * count + 3),
            (where, *[landed[k, m] for m in range(members) for k in half], *held),
            [pltpu.VMEM((members * span, width), BF16), pltpu.VMEM((members * span, inner), BF16)],
            6 * members * span * width * inner,
            16,
        )
        sources = [outs[0], swap(outs[1], "tp", 1)]
        for m in range(2, members, 2):
            there = swap(outs[1 + m // 2], "tp", m)
            sources += [there, swap(there, "tp", 1)]
        merged = call(
            functools.partial(combine_body, sizes),
            [jax.ShapeDtypeStruct((size, width), BF16)] * count,
            [SMEM] + [VMEM] * (count + len(sources)),
            (where, *[landed[k, 0] for k in half], *sources),
            [],
            4 * count * size * 6 * span * width,
            8,
        )
        for k, value in zip(half, merged):
            returned[k] = across(value, k)
    back_pos = call(
        functools.partial(back_body, sizes_all),
        jax.ShapeDtypeStruct((tokens, LANES), F32),
        [SMEM, VMEM],
        (where, ids),
        [],
        1 << 20,
        8,
    )
    ordered = [returned[k] for k in range(n_chunks)]
    moe_out = call(
        final_body,
        jax.ShapeDtypeStruct((tokens, width), BF16),
        [VMEM] * (1 + 2 * n_chunks),
        (back_pos, *ordered, *[swap(value, "tp", 1) for value in ordered]),
        [],
        4 * tokens * tokens * width,
        8,
    )
    return (mixed, moe_out)


def solution(mesh):
    in_specs = (
        P("ep", "tp"),
        P("ep", "tp"),
        P("ep", "tp"),
        P(None, "tp"),
        P("tp"),
        P(),
        P(("ep", "tp"), None),
        P(),
        P(("ep", "tp"), None),
        P(("ep", "tp"), None),
        P(("ep", "tp"), None, None),
        P(("ep", "tp"), None, None),
        P(("ep", "tp"), None, None),
    )
    out_specs = (P(("ep", "tp"), None), P(("ep", "tp"), None))

    return jax.shard_map(shards, mesh=mesh, in_specs=in_specs, out_specs=out_specs, check_vma=False)
```

```python
import functools

import jax
import jax.numpy as jnp
from jax import lax
from jax.experimental import pallas as pl
from jax.experimental.pallas import tpu as pltpu
from jax.sharding import PartitionSpec as P


GROUP_CH = 64
LANES = 128
META = 16
EPS = 1e-06
F32 = jnp.float32
BF16 = jnp.bfloat16


VMEM = pl.BlockSpec(memory_space=pltpu.VMEM)
SMEM = pl.BlockSpec(memory_space=pltpu.SMEM)
HBM = pl.BlockSpec(memory_space=pltpu.HBM)


def dot(a, b):
    return jnp.dot(a, b, preferred_element_type=F32)


def dot_nt(a, b):
    return lax.dot_general(a, b, (((1,), (1,)), ((), ())), preferred_element_type=F32)


def iota(shape, dim):
    return lax.broadcasted_iota(jnp.int32, shape, dim)


def call(body, outs, specs, args, scratch, flops, vmem):
    return pl.pallas_call(
        body,
        out_shape=outs,
        in_specs=specs,
        out_specs=jax.tree.map(lambda _: VMEM, outs),
        scratch_shapes=scratch,
        cost_estimate=pl.CostEstimate(flops=flops, bytes_accessed=1 << 20, transcendentals=0),
        compiler_params=pltpu.CompilerParams(vmem_limit_bytes=vmem << 20),
    )(*args)


def swap(value, axis, mask):
    count = lax.axis_size(axis)
    return lax.ppermute(value, axis, [(i, i ^ mask) for i in range(count)])


def units_of(n_chunks):
    units = 4 if n_chunks >= 4 else 1
    each = n_chunks // units
    return [list(range(u * each, (u + 1) * each)) for u in range(units)]


def fetch(pairs, sems):
    copies = [pltpu.make_async_copy(a, b, sems.at[n]) for n, (a, b) in enumerate(pairs)]
    for copy in copies:
        copy.start()
    return copies


def norm_rows(x_ref, gain, normed, width):
    tokens = x_ref.shape[0]
    step = min(64, tokens)

    def rows(r, carry):
        at = pl.ds(pl.multiple_of(r * step, step), step)
        wide = x_ref[at, :].astype(F32)
        scale = lax.rsqrt(jnp.mean(wide * wide, axis=-1, keepdims=True) + EPS)
        normed[at, :width] = (wide * scale * gain[...]).astype(BF16)
        return carry

    lax.fori_loop(0, tokens // step, rows, 0)


def ranks(sizes, ids, me):
    groups, members, per_group, _ = sizes
    tokens = ids.shape[1]
    experts = -(-groups * members // 16) * 16
    first, second = ids[0:1, :], ids[1:2, :]
    before = (iota((tokens, tokens), 0) < iota((tokens, tokens), 1)).astype(BF16)
    lane = iota((experts, tokens), 0)
    one, two = lane == first, lane == second
    seen = dot((one | two).astype(BF16), before)
    rank_one = jnp.sum(jnp.where(one, seen, 0.0), axis=0, keepdims=True)
    rank_two = jnp.sum(jnp.where(two, seen, 0.0), axis=0, keepdims=True)
    group = first // members
    rank = jnp.sum(jnp.where(lane // members == group, seen, 0.0), axis=0, keepdims=True) * 0.5
    mask = jnp.bitwise_xor(group, me)
    return rank_one, rank_two, (mask // 2) * (2 * per_group) + rank.astype(jnp.int32), jnp.bitwise_and(mask, 1)


def route_rows(sizes, ids, weights, normed, me):
    _, members, _, width = sizes
    tokens = normed.shape[0]
    first, second = ids[0:1, :], ids[1:2, :]
    rank_one, rank_two, base, odd = ranks(sizes, ids, me)
    parts = []
    for k in range(2):
        left = weights[k : k + 1, :]
        for _ in range(3):
            part = left.astype(BF16).astype(F32)
            parts.append(part)
            left = left - part
    row = iota((META, tokens), 0)
    meta = jnp.zeros((META, tokens), F32)
    fields = [(first % members).astype(F32), rank_one, (second % members).astype(F32), rank_two, *parts]
    for at, field in enumerate(fields):
        meta = jnp.where(row == at, field, meta)
    spread = (iota((LANES, META), 0) == iota((LANES, META), 1)).astype(BF16)
    flat = dot(spread, meta.astype(BF16)).astype(BF16)
    ident = (iota((tokens, tokens), 0) == iota((tokens, tokens), 1)).astype(BF16)
    normed[:, width:] = dot_nt(ident, flat).astype(BF16)
    return base, odd


def own_body(sizes, where, x, ids, weights, gain, normed, place):
    base, odd = route_rows(sizes, ids, weights, normed, where[0])
    place[...] = jnp.broadcast_to(jnp.where(odd == where[2], base, -1), place.shape)
    norm_rows(x, gain, normed, sizes[3])


def back_body(sizes, where, ids, pos):
    groups, _, per_group, _ = sizes
    _, _, base, odd = ranks(sizes, ids, where[0])
    back = jnp.where(odd == where[2], base, groups * per_group + base + per_group).astype(F32)
    pos[...] = jnp.broadcast_to(back, (pos.shape[1], pos.shape[0])).T


def prep_body(sizes, where, own, place_own, x_mate, ids_mate, weights_mate, gain, *refs):
    groups, _, per_group, width = sizes
    chunks, mate = refs[:-1], refs[-1]
    base, odd = route_rows(sizes, ids_mate, weights_mate, mate, where[0])
    norm_rows(x_mate, gain, mate, width)
    place_mate = jnp.where(odd == where[2], base + per_group, -1)
    total = groups * per_group
    tokens = mate.shape[0]
    picks = [(iota((total, tokens), 0) == place).astype(BF16) for place in (place_own[0:1, :], place_mate)]
    pick = jnp.concatenate(picks, axis=1)
    block = width // 4
    size = 2 * per_group

    def columns(n, carry):
        cols = pl.ds(pl.multiple_of(n * block, LANES), block)
        out = dot(pick, jnp.concatenate([own[:, cols], mate[:, cols]], axis=0)).astype(BF16)
        for k, ref in enumerate(chunks):
            ref[:, cols] = out[k * size : (k + 1) * size]
        return carry

    lax.fori_loop(0, 4, columns, 0)
    out = dot(pick, jnp.concatenate([own[:, width:], mate[:, width:]], axis=0)).astype(BF16)
    for k, ref in enumerate(chunks):
        ref[:, width:] = out[k * size : (k + 1) * size]


def expert_body(sizes, where, *refs):
    members, per_group, per_expert, width, count = sizes
    landed = [refs[m * count : (m + 1) * count] for m in range(members)]
    gate, up, down = refs[members * count : members * count + 3]
    outs, rows_x, hidden = refs[members * count + 3 : -2], refs[-2], refs[-1]
    me = where[1]
    size = 2 * per_group
    span = count * 2 * per_expert
    block = 512
    pick_row = (iota((META, LANES), 0) == iota((META, LANES), 1)).astype(BF16)
    for m in range(members):
        lanes = jnp.concatenate([r[:, width:] for r in landed[m]], axis=0)
        meta = dot_nt(pick_row, lanes).astype(jnp.int32)
        n = iota((1, count * size), 1)
        base = (n // size) * (2 * per_expert) + ((n % size) // per_group) * per_expert
        at = jnp.where(meta[0:1] == me, base + meta[1:2], jnp.where(meta[2:3] == me, base + meta[3:4], -1))
        pick = (iota((span, count * size), 0) == at).astype(BF16)
        for n in range(width // block):
            cols = slice(n * block, (n + 1) * block)
            value = jnp.concatenate([r[:, cols] for r in landed[m]], axis=0)
            rows_x[m * span : (m + 1) * span, cols] = dot(pick, value).astype(BF16)
    gated = dot(rows_x[...], gate[...])
    upper = dot(rows_x[...], up[...])
    hidden[...] = (gated / (1.0 + jnp.exp(-gated)) * upper).astype(BF16)
    out = dot(hidden[...], down[...]).astype(BF16)
    for m, ref in enumerate(outs):
        ref[...] = out[m * span : (m + 1) * span]


def combine_body(sizes, where, *refs):
    _, per_group, per_expert, width, count = sizes
    metas, sources, outs = refs[:count], refs[count:-count], refs[-count:]
    me = where[1]
    size = 2 * per_group
    span = count * 2 * per_expert
    rows = count * size
    lanes = jnp.concatenate([r[:, width:] for r in metas], axis=0).astype(F32)
    n = iota((rows, 1), 0)
    base = (n // size) * (2 * per_expert) + ((n % size) // per_group) * per_expert
    depth = sum(r.shape[0] for r in sources)
    column = iota((rows, depth), 1)
    picks, weights = [], []
    for k in range(2):
        mask = jnp.bitwise_xor(lanes[:, 2 * k : 2 * k + 1].astype(jnp.int32), me)
        rank = lanes[:, 2 * k + 1 : 2 * k + 2].astype(jnp.int32)
        picks.append((column == mask * span + base + rank).astype(BF16))
        w = 4 + 3 * k
        weights.append(lanes[:, w : w + 1] + lanes[:, w + 1 : w + 2] + lanes[:, w + 2 : w + 3])
    block = 512
    for c in range(width // block):
        cols = slice(c * block, (c + 1) * block)
        value = jnp.concatenate([r[:, cols] for r in sources], axis=0)
        out = (dot(picks[0], value) * weights[0] + dot(picks[1], value) * weights[1]).astype(BF16)
        for k, ref in enumerate(outs):
            ref[:, cols] = out[k * size : (k + 1) * size]


def final_body(pos, *refs):
    sources, out = refs[:-1], refs[-1]
    depth = sum(r.shape[0] for r in sources)
    tokens, width = out.shape
    pick = (iota((tokens, depth), 1) == pos[:, 0:1].astype(jnp.int32)).astype(BF16)
    block = 512
    for c in range(width // block):
        cols = slice(c * block, (c + 1) * block)
        value = jnp.concatenate([r[:, cols] for r in sources], axis=0)
        out[:, cols] = dot(pick, value).astype(BF16)


def conv_body(reach, where, edge, *refs):
    given, outs, taken = refs[:5], refs[5:-8], refs[-8:-3]
    product, normed, sems = refs[-3:]
    copies = fetch(list(zip(given, taken)), sems)
    in_gate, conv_input, out_gate, taps, gain = taken
    me = where[1]
    for copy in copies:
        copy.wait()
    rows, channels = in_gate.shape
    lead = edge.shape[0] // 2
    product[:lead] = edge[:lead].astype(F32) * edge[lead:].astype(F32)
    step = min(128, rows)
    share = (iota((channels, channels), 0) // GROUP_CH == iota((channels, channels), 1) // GROUP_CH).astype(F32) / GROUP_CH
    for r in range(rows // step):
        at = slice(r * step, (r + 1) * step)
        product[lead + r * step : lead + (r + 1) * step] = in_gate[at].astype(F32) * conv_input[at].astype(F32)
    for r in range(rows // step):
        at = slice(r * step, (r + 1) * step)
        total = None
        for tap in range(reach + 1):
            low = lead - reach + tap + r * step
            term = taps[tap : tap + 1, :] * product[low : low + step]
            total = term if total is None else total + term
        gated = out_gate[at].astype(F32) * total
        mean = jnp.dot(gated * gated, share, preferred_element_type=F32, precision=lax.Precision.HIGHEST)
        normed[at] = (gated * lax.rsqrt(mean + EPS) * gain[...]).astype(BF16)
    part = rows // len(outs)
    for m, ref in enumerate(outs):
        ref[...] = normed[pl.ds(pl.multiple_of(jnp.bitwise_xor(me, m) * part, part), part), :]


def mix_body(where, weight, *refs):
    blocks, out = refs[:-1], refs[-1]
    me = where[1]
    channels = blocks[0].shape[1]
    width = out.shape[1]
    block = 512

    def columns(n, carry):
        cols = pl.ds(pl.multiple_of(n * block, block), block)
        total = None
        for m, ref in enumerate(blocks):
            low = pl.multiple_of(jnp.bitwise_xor(me, m) * channels, channels)
            term = dot(ref[...], weight[pl.ds(low, channels), cols])
            total = term if total is None else total + term
        out[:, cols] = total.astype(BF16)
        return carry

    lax.fori_loop(0, width // block, columns, 0)


def shards(
    out_gate,
    in_gate,
    conv_input,
    conv_taps,
    group_gain,
    mix_out_w,
    moe_in,
    moe_gain,
    route_ids,
    route_weight,
    gate_w,
    up_w,
    down_w,
):
    members, groups = lax.axis_size("tp"), lax.axis_size("ep")
    me_ep, me_tp = lax.axis_index("ep"), lax.axis_index("tp")
    where = jnp.stack([me_ep, me_tp, me_tp % 2]).astype(jnp.int32)
    tokens, width = moe_in.shape
    inner = gate_w.shape[2]
    per_group = tokens // groups
    per_expert = 2 * per_group // members
    full = width + LANES
    size = 2 * per_group
    n_chunks = groups // 2

    rows, channels = in_gate.shape
    reach = conv_taps.shape[0] - 1

    x_mate = swap(moe_in, "tp", 1)
    ids, ids_mate = route_ids.T, swap(route_ids.T, "tp", 1)
    weights, weights_mate = route_weight.T, swap(route_weight.T, "tp", 1)
    gain = moe_gain.reshape(1, width)
    sizes_all = (groups, members, per_group, width)
    normed, place = call(
        functools.partial(own_body, sizes_all),
        [jax.ShapeDtypeStruct((tokens, full), BF16), jax.ShapeDtypeStruct((8, tokens), jnp.int32)],
        [SMEM] + [VMEM] * 4,
        (where, moe_in, ids, weights, gain),
        [],
        6 << 30,
        16,
    )
    leaving = call(
        functools.partial(prep_body, sizes_all),
        [jax.ShapeDtypeStruct((size, full), BF16)] * n_chunks,
        [SMEM] + [VMEM] * 6,
        (where, normed, place, x_mate, ids_mate, weights_mate, gain),
        [pltpu.VMEM((tokens, full), BF16)],
        20 << 30,
        16,
    )
    edge = jnp.concatenate([in_gate[rows - 8 :], conv_input[rows - 8 :]], axis=0)
    edge = lax.ppermute(edge, "ep", [(i, i + 1) for i in range(groups - 1)])

    def across(value, k):
        pairs = []
        for i in range(groups):
            for j in range(members):
                mask = 2 * k + j % 2
                if mask:
                    pairs.append((i * members + j, (i ^ mask) * members + j))
        got = lax.ppermute(value, ("ep", "tp"), pairs)
        return jnp.where(me_tp % 2 == 0, value, got) if k == 0 else got

    held = (gate_w[0], up_w[0], down_w[0])
    units = units_of(n_chunks)
    order = range(n_chunks)
    landed = {}
    for k in order:
        landed[k, 0] = across(leaving[k], k)
    for k in order:
        landed[k, 1] = swap(landed[k, 0], "tp", 1)
        for m in range(2, members, 2):
            landed[k, m] = swap(landed[k, 0], "tp", m)
            landed[k, m + 1] = swap(landed[k, m], "tp", 1)

    normed = call(
        functools.partial(conv_body, reach),
        [jax.ShapeDtypeStruct((rows // members, channels), BF16)] * members,
        [SMEM, VMEM] + [HBM] * 5,
        (where, edge, in_gate, conv_input, out_gate, conv_taps, group_gain.reshape(1, channels)),
        [pltpu.VMEM((rows, channels), BF16)] * 3
        + [
            pltpu.VMEM(conv_taps.shape, F32),
            pltpu.VMEM((1, channels), F32),
            pltpu.VMEM((rows + 8, channels), F32),
            pltpu.VMEM((rows, channels), BF16),
            pltpu.SemaphoreType.DMA((5,)),
        ],
        20 << 30,
        8,
    )
    blocks = [normed[0]] + [swap(normed[m], "tp", m) for m in range(1, members)]
    mixed = call(
        mix_body,
        jax.ShapeDtypeStruct((rows // members, width), BF16),
        [SMEM] + [VMEM] * (1 + members),
        (where, mix_out_w, *blocks),
        [],
        2 * (rows // members) * channels * members * width,
        8,
    )

    returned = {}
    for chunks in units:
        count = len(chunks)
        sizes = (members, per_group, per_expert, width, count)
        span = count * 2 * per_expert
        outs = call(
            functools.partial(expert_body, sizes),
            [jax.ShapeDtypeStruct((span, width), BF16)] * members,
            [SMEM] + [VMEM] * (members * count + 3),
            (where, *[landed[k, m] for m in range(members) for k in chunks], *held),
            [pltpu.VMEM((members * span, width), BF16), pltpu.VMEM((members * span, inner), BF16)],
            6 * members * span * width * inner,
            16,
        )
        sources = [outs[0]] + [swap(outs[m], "tp", m) for m in range(1, members)]
        merged = call(
            functools.partial(combine_body, sizes),
            [jax.ShapeDtypeStruct((size, width), BF16)] * count,
            [SMEM] + [VMEM] * (count + members),
            (where, *[landed[k, 0] for k in chunks], *sources),
            [],
            4 * count * size * members * span * width,
            8,
        )
        for k, value in zip(chunks, merged):
            returned[k] = across(value, k)
    back_pos = call(
        functools.partial(back_body, sizes_all),
        jax.ShapeDtypeStruct((tokens, LANES), F32),
        [SMEM, VMEM],
        (where, ids),
        [],
        20 << 30,
        8,
    )
    ordered = [returned[k] for k in range(n_chunks)]
    moe_out = call(
        final_body,
        jax.ShapeDtypeStruct((tokens, width), BF16),
        [VMEM] * (1 + 2 * n_chunks),
        (back_pos, *ordered, *[swap(value, "tp", 1) for value in ordered]),
        [],
        4 * tokens * tokens * width,
        8,
    )
    return (mixed, moe_out)


def solution(mesh):
    in_specs = (
        P("ep", "tp"),
        P("ep", "tp"),
        P("ep", "tp"),
        P(None, "tp"),
        P("tp"),
        P(),
        P(("ep", "tp"), None),
        P(),
        P(("ep", "tp"), None),
        P(("ep", "tp"), None),
        P(("ep", "tp"), None, None),
        P(("ep", "tp"), None, None),
        P(("ep", "tp"), None, None),
    )
    out_specs = (P(("ep", "tp"), None), P(("ep", "tp"), None))

    return jax.shard_map(shards, mesh=mesh, in_specs=in_specs, out_specs=out_specs, check_vma=False)
```

```python
import functools

import jax
import jax.numpy as jnp
from jax import lax
from jax.experimental import pallas as pl
from jax.experimental.pallas import tpu as pltpu
from jax.sharding import PartitionSpec as P


GROUP_CH = 64
LANES = 128
META = 16
EPS = 1e-06
F32 = jnp.float32
BF16 = jnp.bfloat16


VMEM = pl.BlockSpec(memory_space=pltpu.VMEM)
SMEM = pl.BlockSpec(memory_space=pltpu.SMEM)
HBM = pl.BlockSpec(memory_space=pltpu.HBM)


def dot(a, b):
    return jnp.dot(a, b, preferred_element_type=F32)


def dot_nt(a, b):
    return lax.dot_general(a, b, (((1,), (1,)), ((), ())), preferred_element_type=F32)


def iota(shape, dim):
    return lax.broadcasted_iota(jnp.int32, shape, dim)


def call(body, outs, specs, args, scratch, flops, vmem):
    return pl.pallas_call(
        body,
        out_shape=outs,
        in_specs=specs,
        out_specs=jax.tree.map(lambda _: VMEM, outs),
        scratch_shapes=scratch,
        cost_estimate=pl.CostEstimate(flops=flops, bytes_accessed=1 << 20, transcendentals=0),
        compiler_params=pltpu.CompilerParams(vmem_limit_bytes=vmem << 20),
    )(*args)


def swap(value, axis, mask):
    count = lax.axis_size(axis)
    return lax.ppermute(value, axis, [(i, i ^ mask) for i in range(count)])


def units_of(n_chunks):
    units = 4 if n_chunks >= 4 else 1
    each = n_chunks // units
    return [list(range(u * each, (u + 1) * each)) for u in range(units)]


def fetch(pairs, sems):
    copies = [pltpu.make_async_copy(a, b, sems.at[n]) for n, (a, b) in enumerate(pairs)]
    for copy in copies:
        copy.start()
    return copies


def norm_rows(x_ref, gain, normed, width):
    tokens = x_ref.shape[0]
    step = min(64, tokens)

    def rows(r, carry):
        at = pl.ds(pl.multiple_of(r * step, step), step)
        wide = x_ref[at, :].astype(F32)
        scale = lax.rsqrt(jnp.mean(wide * wide, axis=-1, keepdims=True) + EPS)
        normed[at, :width] = (wide * scale * gain[...]).astype(BF16)
        return carry

    lax.fori_loop(0, tokens // step, rows, 0, unroll=True)


def ranks(sizes, route, me):
    groups, members, per_group, _ = sizes
    tokens = route.shape[1]
    experts = -(-groups * members // 16) * 16
    first, second = (route[k : k + 1, :].astype(jnp.int32) for k in range(2))
    before = (iota((tokens, tokens), 0) < iota((tokens, tokens), 1)).astype(BF16)
    lane = iota((experts, tokens), 0)
    one, two = lane == first, lane == second
    seen = dot((one | two).astype(BF16), before)
    rank_one = jnp.sum(jnp.where(one, seen, 0.0), axis=0, keepdims=True)
    rank_two = jnp.sum(jnp.where(two, seen, 0.0), axis=0, keepdims=True)
    group = first // members
    rank = jnp.sum(jnp.where(lane // members == group, seen, 0.0), axis=0, keepdims=True) * 0.5
    mask = jnp.bitwise_xor(group, me)
    return rank_one, rank_two, (mask // 2) * (2 * per_group) + rank.astype(jnp.int32), jnp.bitwise_and(mask, 1)


def route_rows(sizes, route, normed, me):
    _, members, _, width = sizes
    tokens = normed.shape[0]
    first, second = (route[k : k + 1, :].astype(jnp.int32) for k in range(2))
    rank_one, rank_two, base, odd = ranks(sizes, route, me)
    parts = []
    for k in range(2):
        left = route[2 + k : 3 + k, :]
        for _ in range(3):
            part = left.astype(BF16).astype(F32)
            parts.append(part)
            left = left - part
    row = iota((META, tokens), 0)
    meta = jnp.zeros((META, tokens), F32)
    fields = [(first % members).astype(F32), rank_one, (second % members).astype(F32), rank_two, *parts]
    for at, field in enumerate(fields):
        meta = jnp.where(row == at, field, meta)
    spread = (iota((LANES, META), 0) == iota((LANES, META), 1)).astype(BF16)
    flat = dot(spread, meta.astype(BF16)).astype(BF16)
    ident = (iota((tokens, tokens), 0) == iota((tokens, tokens), 1)).astype(BF16)
    normed[:, width:] = dot_nt(ident, flat).astype(BF16)
    return base, odd


def own_body(sizes, where, x, route, gain, normed, place):
    base, odd = route_rows(sizes, route, normed, where[0])
    place[...] = jnp.broadcast_to(jnp.where(odd == where[2], base, -1), place.shape)
    norm_rows(x, gain, normed, sizes[3])


def back_body(sizes, where, route, pos):
    groups, _, per_group, _ = sizes
    _, _, base, odd = ranks(sizes, route, where[0])
    back = jnp.where(odd == where[2], base, groups * per_group + base + per_group).astype(F32)
    pos[...] = jnp.broadcast_to(back, (pos.shape[1], pos.shape[0])).T


def prep_body(sizes, where, own, place_own, x_mate, route_mate, gain, *refs):
    groups, _, per_group, width = sizes
    chunks, mate = refs[:-1], refs[-1]
    base, odd = route_rows(sizes, route_mate, mate, where[0])
    norm_rows(x_mate, gain, mate, width)
    place_mate = jnp.where(odd == where[2], base + per_group, -1)
    total = groups * per_group
    tokens = mate.shape[0]
    picks = [(iota((total, tokens), 0) == place).astype(BF16) for place in (place_own[0:1, :], place_mate)]
    pick = jnp.concatenate(picks, axis=1)
    block = width // 4
    size = 2 * per_group

    def columns(n, carry):
        cols = pl.ds(pl.multiple_of(n * block, LANES), block)
        out = dot(pick, jnp.concatenate([own[:, cols], mate[:, cols]], axis=0)).astype(BF16)
        for k, ref in enumerate(chunks):
            ref[:, cols] = out[k * size : (k + 1) * size]
        return carry

    lax.fori_loop(0, 4, columns, 0, unroll=True)
    out = dot(pick, jnp.concatenate([own[:, width:], mate[:, width:]], axis=0)).astype(BF16)
    for k, ref in enumerate(chunks):
        ref[:, width:] = out[k * size : (k + 1) * size]


def expert_body(sizes, where, *refs):
    members, per_group, per_expert, width, count = sizes
    landed = [refs[m * count : (m + 1) * count] for m in range(members)]
    gate, up, down = refs[members * count : members * count + 3]
    outs, rows_x, hidden = refs[members * count + 3 : -2], refs[-2], refs[-1]
    me = where[1]
    size = 2 * per_group
    span = count * 2 * per_expert
    block = 512
    pick_row = (iota((META, LANES), 0) == iota((META, LANES), 1)).astype(BF16)
    flat = [r for one in landed for r in one]
    meta = dot_nt(pick_row, jnp.concatenate([r[:, width:] for r in flat], axis=0)).astype(jnp.int32)
    total = members * count * size
    n = iota((1, total), 1)
    chunk = (n // (count * size)) * count + (n % (count * size)) // size
    base = chunk * (2 * per_expert) + ((n % size) // per_group) * per_expert
    at = jnp.where(meta[0:1] == me, base + meta[1:2], jnp.where(meta[2:3] == me, base + meta[3:4], -1))
    pick = (iota((members * span, total), 0) == at).astype(BF16)
    for n in range(width // block):
        cols = slice(n * block, (n + 1) * block)
        rows_x[:, cols] = dot(pick, jnp.concatenate([r[:, cols] for r in flat], axis=0)).astype(BF16)
    gated = dot(rows_x[...], gate[...])
    upper = dot(rows_x[...], up[...])
    hidden[...] = (gated / (1.0 + jnp.exp(-gated)) * upper).astype(BF16)
    out = dot(hidden[...], down[...]).astype(BF16)
    for m, ref in enumerate(outs):
        ref[...] = out[m * span : (m + 1) * span]


def combine_body(sizes, where, *refs):
    _, per_group, per_expert, width, count = sizes
    metas, sources, outs = refs[:count], refs[count:-count], refs[-count:]
    me = where[1]
    size = 2 * per_group
    span = count * 2 * per_expert
    rows = count * size
    lanes = jnp.concatenate([r[:, width:] for r in metas], axis=0).astype(F32)
    n = iota((rows, 1), 0)
    base = (n // size) * (2 * per_expert) + ((n % size) // per_group) * per_expert
    depth = sum(r.shape[0] for r in sources)
    column = iota((rows, depth), 1)
    picks, weights = [], []
    for k in range(2):
        mask = jnp.bitwise_xor(lanes[:, 2 * k : 2 * k + 1].astype(jnp.int32), me)
        rank = lanes[:, 2 * k + 1 : 2 * k + 2].astype(jnp.int32)
        picks.append((column == mask * span + base + rank).astype(BF16))
        w = 4 + 3 * k
        weights.append(lanes[:, w : w + 1] + lanes[:, w + 1 : w + 2] + lanes[:, w + 2 : w + 3])
    block = 512
    for c in range(width // block):
        cols = slice(c * block, (c + 1) * block)
        value = jnp.concatenate([r[:, cols] for r in sources], axis=0)
        out = (dot(picks[0], value) * weights[0] + dot(picks[1], value) * weights[1]).astype(BF16)
        for k, ref in enumerate(outs):
            ref[:, cols] = out[k * size : (k + 1) * size]


def final_body(pos, *refs):
    sources, out = refs[:-1], refs[-1]
    depth = sum(r.shape[0] for r in sources)
    tokens, width = out.shape
    pick = (iota((tokens, depth), 1) == pos[:, 0:1].astype(jnp.int32)).astype(BF16)
    block = 512
    for c in range(width // block):
        cols = slice(c * block, (c + 1) * block)
        value = jnp.concatenate([r[:, cols] for r in sources], axis=0)
        out[:, cols] = dot(pick, value).astype(BF16)


def conv_body(reach, where, edge, *refs):
    given, outs, taken = refs[:5], refs[5:-8], refs[-8:-3]
    product, normed, sems = refs[-3:]
    copies = fetch(list(zip(given, taken)), sems)
    in_gate, conv_input, out_gate, taps, gain = taken
    me = where[1]
    for copy in copies:
        copy.wait()
    rows, channels = in_gate.shape
    lead = edge.shape[0] // 2
    product[:lead] = edge[:lead].astype(F32) * edge[lead:].astype(F32)
    step = min(128, rows)
    share = (iota((channels, channels), 0) // GROUP_CH == iota((channels, channels), 1) // GROUP_CH).astype(F32) / GROUP_CH
    for r in range(rows // step):
        at = slice(r * step, (r + 1) * step)
        product[lead + r * step : lead + (r + 1) * step] = in_gate[at].astype(F32) * conv_input[at].astype(F32)
    for r in range(rows // step):
        at = slice(r * step, (r + 1) * step)
        total = None
        for tap in range(reach + 1):
            low = lead - reach + tap + r * step
            term = taps[tap : tap + 1, :] * product[low : low + step]
            total = term if total is None else total + term
        gated = out_gate[at].astype(F32) * total
        mean = jnp.dot(gated * gated, share, preferred_element_type=F32, precision=lax.Precision.HIGHEST)
        normed[at] = (gated * lax.rsqrt(mean + EPS) * gain[...]).astype(BF16)
    part = rows // len(outs)
    for m, ref in enumerate(outs):
        ref[...] = normed[pl.ds(pl.multiple_of(jnp.bitwise_xor(me, m) * part, part), part), :]


def mix_body(where, weight, *refs):
    blocks, out = refs[:-1], refs[-1]
    me = where[1]
    channels = blocks[0].shape[1]
    width = out.shape[1]
    block = 512

    def columns(n, carry):
        cols = pl.ds(pl.multiple_of(n * block, block), block)
        total = None
        for m, ref in enumerate(blocks):
            low = pl.multiple_of(jnp.bitwise_xor(me, m) * channels, channels)
            term = dot(ref[...], weight[pl.ds(low, channels), cols])
            total = term if total is None else total + term
        out[:, cols] = total.astype(BF16)
        return carry

    lax.fori_loop(0, width // block, columns, 0)


def shards(
    out_gate,
    in_gate,
    conv_input,
    conv_taps,
    group_gain,
    mix_out_w,
    moe_in,
    moe_gain,
    route_ids,
    route_weight,
    gate_w,
    up_w,
    down_w,
):
    members, groups = lax.axis_size("tp"), lax.axis_size("ep")
    me_ep, me_tp = lax.axis_index("ep"), lax.axis_index("tp")
    where = jnp.stack([me_ep, me_tp, me_tp % 2]).astype(jnp.int32)
    tokens, width = moe_in.shape
    inner = gate_w.shape[2]
    per_group = tokens // groups
    per_expert = 2 * per_group // members
    full = width + LANES
    size = 2 * per_group
    n_chunks = groups // 2

    rows, channels = in_gate.shape
    reach = conv_taps.shape[0] - 1

    x_mate = swap(moe_in, "tp", 1)
    route = jnp.concatenate([route_ids.astype(F32), route_weight], axis=1).T
    route_mate = swap(route, "tp", 1)
    gain = moe_gain.reshape(1, width)
    sizes_all = (groups, members, per_group, width)
    normed, place = call(
        functools.partial(own_body, sizes_all),
        [jax.ShapeDtypeStruct((tokens, full), BF16), jax.ShapeDtypeStruct((8, tokens), jnp.int32)],
        [SMEM] + [VMEM] * 3,
        (where, moe_in, route, gain),
        [],
        6 << 30,
        16,
    )
    leaving = call(
        functools.partial(prep_body, sizes_all),
        [jax.ShapeDtypeStruct((size, full), BF16)] * n_chunks,
        [SMEM] + [VMEM] * 5,
        (where, normed, place, x_mate, route_mate, gain),
        [pltpu.VMEM((tokens, full), BF16)],
        20 << 30,
        16,
    )
    edge = jnp.concatenate([in_gate[rows - 8 :], conv_input[rows - 8 :]], axis=0)
    edge = lax.ppermute(edge, "ep", [(i, i + 1) for i in range(groups - 1)])

    def across(value, k):
        pairs = []
        for i in range(groups):
            for j in range(members):
                mask = 2 * k + j % 2
                if mask:
                    pairs.append((i * members + j, (i ^ mask) * members + j))
        got = lax.ppermute(value, ("ep", "tp"), pairs)
        return jnp.where(me_tp % 2 == 0, value, got) if k == 0 else got

    held = (gate_w[0], up_w[0], down_w[0])
    units = units_of(n_chunks)
    order = range(n_chunks)
    landed = {}
    for k in order:
        landed[k, 0] = across(leaving[k], k)
    for k in order:
        landed[k, 1] = swap(landed[k, 0], "tp", 1)
        for m in range(2, members, 2):
            landed[k, m] = swap(landed[k, 0], "tp", m)
            landed[k, m + 1] = swap(landed[k, m], "tp", 1)

    normed = call(
        functools.partial(conv_body, reach),
        [jax.ShapeDtypeStruct((rows // members, channels), BF16)] * members,
        [SMEM, VMEM] + [HBM] * 5,
        (where, edge, in_gate, conv_input, out_gate, conv_taps, group_gain.reshape(1, channels)),
        [pltpu.VMEM((rows, channels), BF16)] * 3
        + [
            pltpu.VMEM(conv_taps.shape, F32),
            pltpu.VMEM((1, channels), F32),
            pltpu.VMEM((rows + 8, channels), F32),
            pltpu.VMEM((rows, channels), BF16),
            pltpu.SemaphoreType.DMA((5,)),
        ],
        20 << 30,
        8,
    )
    blocks = [normed[0]] + [swap(normed[m], "tp", m) for m in range(1, members)]
    mixed = call(
        mix_body,
        jax.ShapeDtypeStruct((rows // members, width), BF16),
        [SMEM] + [VMEM] * (1 + members),
        (where, mix_out_w, *blocks),
        [],
        2 * (rows // members) * channels * members * width,
        8,
    )

    returned = {}
    for chunks in units:
        count = len(chunks)
        sizes = (members, per_group, per_expert, width, count)
        span = count * 2 * per_expert
        outs = call(
            functools.partial(expert_body, sizes),
            [jax.ShapeDtypeStruct((span, width), BF16)] * members,
            [SMEM] + [VMEM] * (members * count + 3),
            (where, *[landed[k, m] for m in range(members) for k in chunks], *held),
            [pltpu.VMEM((members * span, width), BF16), pltpu.VMEM((members * span, inner), BF16)],
            6 * members * span * width * inner,
            16,
        )
        sources = [outs[0]] + [swap(outs[m], "tp", m) for m in range(1, members)]
        merged = call(
            functools.partial(combine_body, sizes),
            [jax.ShapeDtypeStruct((size, width), BF16)] * count,
            [SMEM] + [VMEM] * (count + members),
            (where, *[landed[k, 0] for k in chunks], *sources),
            [],
            4 * count * size * members * span * width,
            8,
        )
        for k, value in zip(chunks, merged):
            returned[k] = across(value, k)
    back_pos = call(
        functools.partial(back_body, sizes_all),
        jax.ShapeDtypeStruct((tokens, LANES), F32),
        [SMEM, VMEM],
        (where, route),
        [],
        20 << 30,
        8,
    )
    ordered = [returned[k] for k in range(n_chunks)]
    moe_out = call(
        final_body,
        jax.ShapeDtypeStruct((tokens, width), BF16),
        [VMEM] * (1 + 2 * n_chunks),
        (back_pos, *ordered, *[swap(value, "tp", 1) for value in ordered]),
        [],
        4 * tokens * tokens * width,
        8,
    )
    return (mixed, moe_out)


def solution(mesh):
    in_specs = (
        P("ep", "tp"),
        P("ep", "tp"),
        P("ep", "tp"),
        P(None, "tp"),
        P("tp"),
        P(),
        P(("ep", "tp"), None),
        P(),
        P(("ep", "tp"), None),
        P(("ep", "tp"), None),
        P(("ep", "tp"), None, None),
        P(("ep", "tp"), None, None),
        P(("ep", "tp"), None, None),
    )
    out_specs = (P(("ep", "tp"), None), P(("ep", "tp"), None))

    return jax.shard_map(shards, mesh=mesh, in_specs=in_specs, out_specs=out_specs, check_vma=False)
```

```python
import functools

import jax
import jax.numpy as jnp
from jax import lax
from jax.experimental import pallas as pl
from jax.experimental.pallas import tpu as pltpu
from jax.sharding import PartitionSpec as P


GROUP_CH = 64
LANES = 128
META = 16
EPS = 1e-06
F32 = jnp.float32
BF16 = jnp.bfloat16


VMEM = pl.BlockSpec(memory_space=pltpu.VMEM)
SMEM = pl.BlockSpec(memory_space=pltpu.SMEM)
HBM = pl.BlockSpec(memory_space=pltpu.HBM)


def dot(a, b):
    return jnp.dot(a, b, preferred_element_type=F32)


def dot_nt(a, b):
    return lax.dot_general(a, b, (((1,), (1,)), ((), ())), preferred_element_type=F32)


def iota(shape, dim):
    return lax.broadcasted_iota(jnp.int32, shape, dim)


def call(body, outs, specs, args, scratch, flops, vmem, place=VMEM):
    return pl.pallas_call(
        body,
        out_shape=outs,
        in_specs=specs,
        out_specs=jax.tree.map(lambda _: place, outs),
        scratch_shapes=scratch,
        cost_estimate=pl.CostEstimate(flops=flops, bytes_accessed=1 << 20, transcendentals=0),
        compiler_params=pltpu.CompilerParams(vmem_limit_bytes=vmem << 20),
    )(*args)


def swap(value, axis, mask):
    count = lax.axis_size(axis)
    return lax.ppermute(value, axis, [(i, i ^ mask) for i in range(count)])


def units_of(n_chunks):
    units = 4 if n_chunks >= 4 else 1
    each = n_chunks // units
    return [list(range(u * each, (u + 1) * each)) for u in range(units)]


def fetch(pairs, sems):
    copies = [pltpu.make_async_copy(a, b, sems.at[n]) for n, (a, b) in enumerate(pairs)]
    for copy in copies:
        copy.start()
    return copies


def norm_rows(x_ref, gain, normed, width):
    tokens = x_ref.shape[0]
    step = min(64, tokens)

    def rows(r, carry):
        at = pl.ds(pl.multiple_of(r * step, step), step)
        wide = x_ref[at, :].astype(F32)
        scale = lax.rsqrt(jnp.mean(wide * wide, axis=-1, keepdims=True) + EPS)
        normed[at, :width] = (wide * scale * gain[...]).astype(BF16)
        return carry

    lax.fori_loop(0, tokens // step, rows, 0, unroll=True)


def ranks(sizes, route, me):
    groups, members, per_group, _ = sizes
    tokens = route.shape[1]
    experts = -(-groups * members // 16) * 16
    first, second = (route[k : k + 1, :].astype(jnp.int32) for k in range(2))
    before = (iota((tokens, tokens), 0) < iota((tokens, tokens), 1)).astype(BF16)
    lane = iota((experts, tokens), 0)
    one, two = lane == first, lane == second
    seen = dot((one | two).astype(BF16), before)
    rank_one = jnp.sum(jnp.where(one, seen, 0.0), axis=0, keepdims=True)
    rank_two = jnp.sum(jnp.where(two, seen, 0.0), axis=0, keepdims=True)
    group = first // members
    rank = jnp.sum(jnp.where(lane // members == group, seen, 0.0), axis=0, keepdims=True) * 0.5
    mask = jnp.bitwise_xor(group, me)
    return rank_one, rank_two, (mask // 2) * (2 * per_group) + rank.astype(jnp.int32), jnp.bitwise_and(mask, 1)


def route_rows(sizes, route, normed, me):
    _, members, _, width = sizes
    tokens = normed.shape[0]
    first, second = (route[k : k + 1, :].astype(jnp.int32) for k in range(2))
    rank_one, rank_two, base, odd = ranks(sizes, route, me)
    parts = []
    for k in range(2):
        left = route[2 + k : 3 + k, :]
        for _ in range(3):
            part = left.astype(BF16).astype(F32)
            parts.append(part)
            left = left - part
    row = iota((META, tokens), 0)
    meta = jnp.zeros((META, tokens), F32)
    fields = [(first % members).astype(F32), rank_one, (second % members).astype(F32), rank_two, *parts]
    for at, field in enumerate(fields):
        meta = jnp.where(row == at, field, meta)
    spread = (iota((LANES, META), 0) == iota((LANES, META), 1)).astype(BF16)
    flat = dot(spread, meta.astype(BF16)).astype(BF16)
    ident = (iota((tokens, tokens), 0) == iota((tokens, tokens), 1)).astype(BF16)
    normed[:, width:] = dot_nt(ident, flat).astype(BF16)
    return base, odd


def own_body(sizes, where, x, route, gain, normed, place):
    base, odd = route_rows(sizes, route, normed, where[0])
    place[...] = jnp.broadcast_to(jnp.where(odd == where[2], base, -1), place.shape)
    norm_rows(x, gain, normed, sizes[3])


def back_body(sizes, where, route, pos):
    groups, _, per_group, _ = sizes
    _, _, base, odd = ranks(sizes, route, where[0])
    back = jnp.where(odd == where[2], base, groups * per_group + base + per_group).astype(F32)
    pos[...] = jnp.broadcast_to(back, (pos.shape[1], pos.shape[0])).T


def prep_body(sizes, where, own, place_own, x_mate, route_mate, gain, *refs):
    groups, _, per_group, width = sizes
    chunks, mate = refs[:-1], refs[-1]
    base, odd = route_rows(sizes, route_mate, mate, where[0])
    norm_rows(x_mate, gain, mate, width)
    place_mate = jnp.where(odd == where[2], base + per_group, -1)
    total = groups * per_group
    tokens = mate.shape[0]
    picks = [(iota((total, tokens), 0) == place).astype(BF16) for place in (place_own[0:1, :], place_mate)]
    pick = jnp.concatenate(picks, axis=1)
    block = width // 4
    size = 2 * per_group

    def columns(n, carry):
        cols = pl.ds(pl.multiple_of(n * block, LANES), block)
        out = dot(pick, jnp.concatenate([own[:, cols], mate[:, cols]], axis=0)).astype(BF16)
        for k, ref in enumerate(chunks):
            ref[:, cols] = out[k * size : (k + 1) * size]
        return carry

    lax.fori_loop(0, 4, columns, 0, unroll=True)
    out = dot(pick, jnp.concatenate([own[:, width:], mate[:, width:]], axis=0)).astype(BF16)
    for k, ref in enumerate(chunks):
        ref[:, width:] = out[k * size : (k + 1) * size]


def expert_body(sizes, where, *refs):
    members, per_group, per_expert, width, count = sizes
    landed = [refs[m * count : (m + 1) * count] for m in range(members)]
    gate, up, down = refs[members * count : members * count + 3]
    outs, rows_x, hidden = refs[members * count + 3 : -2], refs[-2], refs[-1]
    me = where[1]
    size = 2 * per_group
    span = count * 2 * per_expert
    block = 512
    pick_row = (iota((META, LANES), 0) == iota((META, LANES), 1)).astype(BF16)
    flat = [r for one in landed for r in one]
    meta = dot_nt(pick_row, jnp.concatenate([r[:, width:] for r in flat], axis=0)).astype(jnp.int32)
    total = members * count * size
    n = iota((1, total), 1)
    chunk = (n // (count * size)) * count + (n % (count * size)) // size
    base = chunk * (2 * per_expert) + ((n % size) // per_group) * per_expert
    at = jnp.where(meta[0:1] == me, base + meta[1:2], jnp.where(meta[2:3] == me, base + meta[3:4], -1))
    pick = (iota((members * span, total), 0) == at).astype(BF16)
    for n in range(width // block):
        cols = slice(n * block, (n + 1) * block)
        rows_x[:, cols] = dot(pick, jnp.concatenate([r[:, cols] for r in flat], axis=0)).astype(BF16)
    gated = dot(rows_x[...], gate[...])
    upper = dot(rows_x[...], up[...])
    hidden[...] = (gated / (1.0 + jnp.exp(-gated)) * upper).astype(BF16)
    out = dot(hidden[...], down[...]).astype(BF16)
    for m, ref in enumerate(outs):
        ref[...] = out[m * span : (m + 1) * span]


def combine_body(sizes, where, *refs):
    _, per_group, per_expert, width, count = sizes
    metas, sources, outs = refs[:count], refs[count:-count], refs[-count:]
    me = where[1]
    size = 2 * per_group
    span = count * 2 * per_expert
    rows = count * size
    lanes = jnp.concatenate([r[:, width:] for r in metas], axis=0).astype(F32)
    n = iota((rows, 1), 0)
    base = (n // size) * (2 * per_expert) + ((n % size) // per_group) * per_expert
    depth = sum(r.shape[0] for r in sources)
    column = iota((rows, depth), 1)
    picks, weights = [], []
    for k in range(2):
        mask = jnp.bitwise_xor(lanes[:, 2 * k : 2 * k + 1].astype(jnp.int32), me)
        rank = lanes[:, 2 * k + 1 : 2 * k + 2].astype(jnp.int32)
        picks.append((column == mask * span + base + rank).astype(BF16))
        w = 4 + 3 * k
        weights.append(lanes[:, w : w + 1] + lanes[:, w + 1 : w + 2] + lanes[:, w + 2 : w + 3])
    block = 512
    for c in range(width // block):
        cols = slice(c * block, (c + 1) * block)
        value = jnp.concatenate([r[:, cols] for r in sources], axis=0)
        out = (dot(picks[0], value) * weights[0] + dot(picks[1], value) * weights[1]).astype(BF16)
        for k, ref in enumerate(outs):
            ref[:, cols] = out[k * size : (k + 1) * size]


def final_body(pos, *refs):
    sources, out, built, sems = refs[:-3], refs[-3], refs[-2], refs[-1]
    depth = sum(r.shape[0] for r in sources)
    tokens, width = out.shape
    pick = (iota((tokens, depth), 1) == pos[:, 0:1].astype(jnp.int32)).astype(BF16)
    block = 512
    copies = []
    for c in range(width // block):
        cols = slice(c * block, (c + 1) * block)
        value = jnp.concatenate([r[:, cols] for r in sources], axis=0)
        built[:, cols] = dot(pick, value).astype(BF16)
        at = pl.ds(c * block, block)
        copies.append(pltpu.make_async_copy(built.at[:, at], out.at[:, at], sems.at[c]))
        copies[-1].start()
    for copy in copies:
        copy.wait()


def conv_body(reach, where, edge, *refs):
    given, outs, taken = refs[:5], refs[5:-8], refs[-8:-3]
    product, normed, sems = refs[-3:]
    copies = fetch(list(zip(given, taken)), sems)
    in_gate, conv_input, out_gate, taps, gain = taken
    me = where[1]
    for copy in copies:
        copy.wait()
    rows, channels = in_gate.shape
    lead = edge.shape[0] // 2
    product[:lead] = edge[:lead].astype(F32) * edge[lead:].astype(F32)
    step = min(128, rows)
    share = (iota((channels, channels), 0) // GROUP_CH == iota((channels, channels), 1) // GROUP_CH).astype(F32) / GROUP_CH
    for r in range(rows // step):
        at = slice(r * step, (r + 1) * step)
        product[lead + r * step : lead + (r + 1) * step] = in_gate[at].astype(F32) * conv_input[at].astype(F32)
    for r in range(rows // step):
        at = slice(r * step, (r + 1) * step)
        total = None
        for tap in range(reach + 1):
            low = lead - reach + tap + r * step
            term = taps[tap : tap + 1, :] * product[low : low + step]
            total = term if total is None else total + term
        gated = out_gate[at].astype(F32) * total
        mean = jnp.dot(gated * gated, share, preferred_element_type=F32, precision=lax.Precision.HIGHEST)
        normed[at] = (gated * lax.rsqrt(mean + EPS) * gain[...]).astype(BF16)
    part = rows // len(outs)
    for m, ref in enumerate(outs):
        ref[...] = normed[pl.ds(pl.multiple_of(jnp.bitwise_xor(me, m) * part, part), part), :]


def mix_body(where, weight, *refs):
    blocks, out = refs[:-1], refs[-1]
    me = where[1]
    channels = blocks[0].shape[1]
    width = out.shape[1]
    block = 512

    def columns(n, carry):
        cols = pl.ds(pl.multiple_of(n * block, block), block)
        total = None
        for m, ref in enumerate(blocks):
            low = pl.multiple_of(jnp.bitwise_xor(me, m) * channels, channels)
            term = dot(ref[...], weight[pl.ds(low, channels), cols])
            total = term if total is None else total + term
        out[:, cols] = total.astype(BF16)
        return carry

    lax.fori_loop(0, width // block, columns, 0, unroll=True)


def shards(
    out_gate,
    in_gate,
    conv_input,
    conv_taps,
    group_gain,
    mix_out_w,
    moe_in,
    moe_gain,
    route_ids,
    route_weight,
    gate_w,
    up_w,
    down_w,
):
    members, groups = lax.axis_size("tp"), lax.axis_size("ep")
    me_ep, me_tp = lax.axis_index("ep"), lax.axis_index("tp")
    where = jnp.stack([me_ep, me_tp, me_tp % 2]).astype(jnp.int32)
    tokens, width = moe_in.shape
    inner = gate_w.shape[2]
    per_group = tokens // groups
    per_expert = 2 * per_group // members
    full = width + LANES
    size = 2 * per_group
    n_chunks = groups // 2

    rows, channels = in_gate.shape
    reach = conv_taps.shape[0] - 1

    x_mate = swap(moe_in, "tp", 1)
    route = jnp.concatenate([route_ids.astype(F32), route_weight], axis=1).T
    route_mate = swap(route, "tp", 1)
    gain = moe_gain.reshape(1, width)
    sizes_all = (groups, members, per_group, width)
    normed, place = call(
        functools.partial(own_body, sizes_all),
        [jax.ShapeDtypeStruct((tokens, full), BF16), jax.ShapeDtypeStruct((8, tokens), jnp.int32)],
        [SMEM] + [VMEM] * 3,
        (where, moe_in, route, gain),
        [],
        6 << 30,
        16,
    )
    leaving = call(
        functools.partial(prep_body, sizes_all),
        [jax.ShapeDtypeStruct((size, full), BF16)] * n_chunks,
        [SMEM] + [VMEM] * 5,
        (where, normed, place, x_mate, route_mate, gain),
        [pltpu.VMEM((tokens, full), BF16)],
        20 << 30,
        16,
    )
    edge = jnp.concatenate([in_gate[rows - 8 :], conv_input[rows - 8 :]], axis=0)
    edge = lax.ppermute(edge, "ep", [(i, i + 1) for i in range(groups - 1)])

    def across(value, k):
        pairs = []
        for i in range(groups):
            for j in range(members):
                mask = 2 * k + j % 2
                if mask:
                    pairs.append((i * members + j, (i ^ mask) * members + j))
        got = lax.ppermute(value, ("ep", "tp"), pairs)
        return jnp.where(me_tp % 2 == 0, value, got) if k == 0 else got

    held = (gate_w[0], up_w[0], down_w[0])
    units = units_of(n_chunks)
    order = range(n_chunks)
    landed = {}
    for k in order:
        landed[k, 0] = across(leaving[k], k)
    for k in order:
        landed[k, 1] = swap(landed[k, 0], "tp", 1)
        for m in range(2, members, 2):
            landed[k, m] = swap(landed[k, 0], "tp", m)
            landed[k, m + 1] = swap(landed[k, m], "tp", 1)

    normed = call(
        functools.partial(conv_body, reach),
        [jax.ShapeDtypeStruct((rows // members, channels), BF16)] * members,
        [SMEM, VMEM] + [HBM] * 5,
        (where, edge, in_gate, conv_input, out_gate, conv_taps, group_gain.reshape(1, channels)),
        [pltpu.VMEM((rows, channels), BF16)] * 3
        + [
            pltpu.VMEM(conv_taps.shape, F32),
            pltpu.VMEM((1, channels), F32),
            pltpu.VMEM((rows + 8, channels), F32),
            pltpu.VMEM((rows, channels), BF16),
            pltpu.SemaphoreType.DMA((5,)),
        ],
        20 << 30,
        8,
    )
    blocks = [normed[0]] + [swap(normed[m], "tp", m) for m in range(1, members)]
    mixed = call(
        mix_body,
        jax.ShapeDtypeStruct((rows // members, width), BF16),
        [SMEM] + [VMEM] * (1 + members),
        (where, mix_out_w, *blocks),
        [],
        2 * (rows // members) * channels * members * width,
        8,
    )

    returned = {}
    for chunks in units:
        count = len(chunks)
        sizes = (members, per_group, per_expert, width, count)
        span = count * 2 * per_expert
        outs = call(
            functools.partial(expert_body, sizes),
            [jax.ShapeDtypeStruct((span, width), BF16)] * members,
            [SMEM] + [VMEM] * (members * count + 3),
            (where, *[landed[k, m] for m in range(members) for k in chunks], *held),
            [pltpu.VMEM((members * span, width), BF16), pltpu.VMEM((members * span, inner), BF16)],
            6 * members * span * width * inner,
            16,
        )
        sources = [outs[0]] + [swap(outs[m], "tp", m) for m in range(1, members)]
        merged = call(
            functools.partial(combine_body, sizes),
            [jax.ShapeDtypeStruct((size, width), BF16)] * count,
            [SMEM] + [VMEM] * (count + members),
            (where, *[landed[k, 0] for k in chunks], *sources),
            [],
            4 * count * size * members * span * width,
            8,
        )
        for k, value in zip(chunks, merged):
            returned[k] = across(value, k)
    back_pos = call(
        functools.partial(back_body, sizes_all),
        jax.ShapeDtypeStruct((tokens, LANES), F32),
        [SMEM, VMEM],
        (where, route),
        [],
        20 << 30,
        8,
    )
    ordered = [returned[k] for k in range(n_chunks)]
    moe_out = call(
        final_body,
        jax.ShapeDtypeStruct((tokens, width), BF16),
        [VMEM] * (1 + 2 * n_chunks),
        (back_pos, *ordered, *[swap(value, "tp", 1) for value in ordered]),
        [pltpu.VMEM((tokens, width), BF16), pltpu.SemaphoreType.DMA((width // 512,))],
        4 * tokens * tokens * width,
        8,
        HBM,
    )
    return (mixed, moe_out)


def solution(mesh):
    in_specs = (
        P("ep", "tp"),
        P("ep", "tp"),
        P("ep", "tp"),
        P(None, "tp"),
        P("tp"),
        P(),
        P(("ep", "tp"), None),
        P(),
        P(("ep", "tp"), None),
        P(("ep", "tp"), None),
        P(("ep", "tp"), None, None),
        P(("ep", "tp"), None, None),
        P(("ep", "tp"), None, None),
    )
    out_specs = (P(("ep", "tp"), None), P(("ep", "tp"), None))

    return jax.shard_map(shards, mesh=mesh, in_specs=in_specs, out_specs=out_specs, check_vma=False)
```
